32 devices in a mesh: fs: 16 (over z, y, x), tp: 2 (over core).
Axes of the slice: x: 2, y: 2, z: 4, core: 2. Of those that a mesh axis runs over, the one named last changes fastest.
Arguments:
- sequence_entries: bfloat16 [4096, 2048], P('fs', 'tp'), may hold values from -6 to 6
- former_norm_factor: float32 [2048], replicated, may hold values from 0.1 to 1.9
- conveyor_matrix: float32 [2048, 1536], P('fs', 'tp'), may hold values from -0.125 to 0.125
- conveyor_rescalers: float32 [1536], P('tp'), may hold values from 0.3 to 3
- blend_value_matrix: float32 [2048, 1536], P('fs', 'tp'), may hold values from -0.125 to 0.125
- blend_rescalers: float32 [1536], P('tp'), may hold values from 0.18 to 4.8, as said below
- blend_norm_factor: float32 [1536], P('tp'), may hold values from 0.1 to 1.9
- location_matrices: bfloat16 [24, 128, 128], P('tp'), may hold values from -0.5 to 0.5
- location_offsets: float32 [24, 128], P('tp'), may hold values from 0.1 to 1.9
- branch_emission_matrix: float32 [1536, 2048], P('tp', 'fs'), may hold values from -0.15625 to 0.15625
- emission_rescalers: float32 [2048], P('fs'), may hold values from 0.3 to 3
- latter_norm_factor: float32 [2048], replicated, may hold values from 0.1 to 1.9
- valve_matrix: float32 [2048, 5632], P('fs', 'tp'), may hold values from -0.125 to 0.125
- valve_rescalers: float32 [5632], P('tp'), may hold values from 0.3 to 3
- raising_matrix: float32 [2048, 5632], P('fs', 'tp'), may hold values from -0.125 to 0.125
- raising_rescalers: float32 [5632], P('tp'), may hold values from 0.3 to 3
- lowering_matrix: float32 [5632, 2048], P('tp', 'fs'), may hold values from -0.078125 to 0.078125
- lowering_rescalers: float32 [2048], P('fs'), may hold values from 0.3 to 3
Outputs:
- layer_out: bfloat16 [4096, 2048], P('fs', 'tp')
The draws below stay inside these ranges and needn't reach their ends.
Inputs may be any that keep to these rules, and one draw needn't show every extreme that they name: `blend_rescalers`: positive column scales.
All inputs are finite; a program needn't handle non-finite values.
Results may differ from the reference program's by a relative error of at most 0.02.
Values may be sent and summed in bfloat16 or wider, within the bound.
A program may use at most 128 MiB of HBM per device.

```python
import math
import jax
import jax.numpy as jnp
from jax import lax

MODEL_BREADTH = 2048
FILTER_BUNDLES = 24
BUNDLE_BREADTH = 64
BLEND_BREADTH = 1536
FF = 5632
BLOCK = 128
WORD_TOTALITY = 4096
N_TP = 2


def draw_blend_rescalers(key, part):
    noise_key = jax.random.fold_in(key, 11)
    place = jnp.arange(BLEND_BREADTH, dtype=jnp.float32) / max(BLEND_BREADTH - 1, 1)
    jitter = jnp.exp(jax.random.uniform(noise_key, (BLEND_BREADTH,), jnp.float32, math.log(0.6), math.log(1.6)))
    ramp = jnp.exp(math.log(0.4) + place * math.log(5.0))
    return (ramp * jitter).astype(jnp.float32)


def shard_levels(key, shape, split, least, high):
    level, own = 1.0, jax.random.fold_in(key, 6)
    for axis_at, parts in split:
        heights = jnp.exp(jax.random.uniform(jax.random.fold_in(own, axis_at), (parts,), jnp.float32, least / len(split), high / len(split)))
        level = level * jnp.repeat(heights, shape[axis_at] // parts).reshape([-1 if axis == axis_at else 1 for axis in range(len(shape))])
    return level


def scatter_about(stream_key, extent, deviation, most, shards=(), kind=jnp.bfloat16):
    array = jax.random.normal(stream_key, extent, jnp.float32) * deviation
    if len(shards) > 0:
        array = shard_levels(stream_key, extent, shards, -0.22, 0.18) * array
    return jnp.clip(array, min=-most, max=most).astype(kind)


def setup_inputs(seed: int = 0) -> dict:
    key_of = jax.random.split(jax.random.key(seed), 19)
    sequence_entries = scatter_about(key_of[0], (WORD_TOTALITY, MODEL_BREADTH), 1.0, 6.0, ((0, 16), (1, 2)))
    former_norm_factor = jnp.clip(1.0 + 0.18 * jax.random.normal(key_of[1], (MODEL_BREADTH,), jnp.float32), 0.1, 1.9)
    conveyor_matrix = scatter_about(key_of[2], (MODEL_BREADTH, BLEND_BREADTH), MODEL_BREADTH ** -0.5, 0.125, ((0, 16), (1, 2)), jnp.float32)
    conveyor_rescalers = jnp.clip(jnp.exp(math.log(3.0) - 2.3025851 * jax.random.uniform(key_of[3], (BLEND_BREADTH,), jnp.float32) ** shard_levels(key_of[3], (BLEND_BREADTH,), ((0, 2),), -0.2, 0.2)), 0.3, 3.0)
    blend_value_matrix = scatter_about(key_of[4], (MODEL_BREADTH, BLEND_BREADTH), MODEL_BREADTH ** -0.5, 0.125, ((0, 16), (1, 2)), jnp.float32)
    blend_rescalers = draw_blend_rescalers(jax.random.fold_in(key_of[18], 71), 0)
    blend_norm_factor = jnp.clip(1.0 + 0.18 * jax.random.normal(key_of[6], (BLEND_BREADTH,), jnp.float32), 0.1, 1.9)
    location_matrices = scatter_about(key_of[7], (FILTER_BUNDLES, BLOCK, BLOCK), BLOCK ** -0.5, 0.5, ((0, 2),))
    location_offsets = jnp.clip(1.0 + 0.18 * jax.random.normal(key_of[8], (FILTER_BUNDLES, BLOCK), jnp.float32), 0.1, 1.9)
    branch_emission_matrix = scatter_about(key_of[9], (BLEND_BREADTH, MODEL_BREADTH), BLEND_BREADTH ** -0.5, 0.15625, ((0, 2), (1, 16)), jnp.float32)
    emission_rescalers = jnp.clip(jnp.exp(math.log(3.0) - 2.3025851 * jax.random.uniform(key_of[10], (MODEL_BREADTH,), jnp.float32) ** shard_levels(key_of[10], (MODEL_BREADTH,), ((0, 16),), -0.2, 0.2)), 0.3, 3.0)
    latter_norm_factor = jnp.clip(1.0 + 0.18 * jax.random.normal(key_of[11], (MODEL_BREADTH,), jnp.float32), 0.1, 1.9)
    valve_matrix = scatter_about(key_of[12], (MODEL_BREADTH, FF), MODEL_BREADTH ** -0.5, 0.125, ((0, 16), (1, 2)), jnp.float32)
    valve_rescalers = jnp.clip(jnp.exp(math.log(3.0) - 2.3025851 * jax.random.uniform(key_of[13], (FF,), jnp.float32) ** shard_levels(key_of[13], (FF,), ((0, 2),), -0.2, 0.2)), 0.3, 3.0)
    raising_matrix = scatter_about(key_of[14], (MODEL_BREADTH, FF), MODEL_BREADTH ** -0.5, 0.125, ((0, 16), (1, 2)), jnp.float32)
    raising_rescalers = jnp.clip(jnp.exp(math.log(3.0) - 2.3025851 * jax.random.uniform(key_of[15], (FF,), jnp.float32) ** shard_levels(key_of[15], (FF,), ((0, 2),), -0.2, 0.2)), 0.3, 3.0)
    lowering_matrix = scatter_about(key_of[16], (FF, MODEL_BREADTH), FF ** -0.5, 0.078125, ((0, 2), (1, 16)), jnp.float32)
    lowering_rescalers = jnp.clip(jnp.exp(math.log(3.0) - 2.3025851 * jax.random.uniform(key_of[17], (MODEL_BREADTH,), jnp.float32) ** shard_levels(key_of[17], (MODEL_BREADTH,), ((0, 16),), -0.2, 0.2)), 0.3, 3.0)
    return dict(sequence_entries=sequence_entries, former_norm_factor=former_norm_factor, conveyor_matrix=conveyor_matrix, conveyor_rescalers=conveyor_rescalers, blend_value_matrix=blend_value_matrix, blend_rescalers=blend_rescalers, blend_norm_factor=blend_norm_factor, location_matrices=location_matrices, location_offsets=location_offsets, branch_emission_matrix=branch_emission_matrix, emission_rescalers=emission_rescalers, latter_norm_factor=latter_norm_factor, valve_matrix=valve_matrix, valve_rescalers=valve_rescalers, raising_matrix=raising_matrix, raising_rescalers=raising_rescalers, lowering_matrix=lowering_matrix, lowering_rescalers=lowering_rescalers)


EPS = 1e-06

def normalize(rows, gain):
    values = rows.astype(jnp.float32)
    factor = lax.rsqrt(lax.optimization_barrier(jnp.mean(values * values, axis=-1, keepdims=True)) + EPS)
    return (values * factor * gain).astype(jnp.bfloat16)

def rescaled_matmul(left, weight, scale):
    return jnp.dot(left, weight.astype(jnp.bfloat16), preferred_element_type=jnp.float32) * scale

def split_sum(left, weight, scale, groups):
    width = left.shape[1] // groups
    total = jnp.zeros((left.shape[0], weight.shape[1]), jnp.float32)
    for index in range(groups):
        part_sum = rescaled_matmul(left[:, index * width:(index + 1) * width], weight[index * width:(index + 1) * width], scale).astype(jnp.bfloat16)
        part_sum = lax.optimization_barrier(part_sum)
        total = total + part_sum.astype(jnp.float32)
    return total

def reference(sequence_entries, former_norm_factor, conveyor_matrix, conveyor_rescalers, blend_value_matrix, blend_rescalers, blend_norm_factor, location_matrices, location_offsets, branch_emission_matrix, emission_rescalers, latter_norm_factor, valve_matrix, valve_rescalers, raising_matrix, raising_rescalers, lowering_matrix, lowering_rescalers):
    standardized_source = normalize(sequence_entries, former_norm_factor)
    conveyor_current = jax.nn.gelu(rescaled_matmul(standardized_source, conveyor_matrix, conveyor_rescalers))
    signal = jax.nn.gelu(rescaled_matmul(standardized_source, blend_value_matrix, blend_rescalers))
    factor = lax.rsqrt(lax.optimization_barrier(jnp.mean(signal * signal, axis=-1, keepdims=True)) + EPS)
    signal_norm = (signal * factor * blend_norm_factor).astype(jnp.bfloat16)
    lower_mask = jnp.tril(jnp.ones((BLOCK, BLOCK), bool))
    masked = jnp.where(lower_mask[None], location_matrices.astype(jnp.float32), jnp.float32(0.0))
    signal_blocks = signal_norm.astype(jnp.float32).reshape(WORD_TOTALITY // BLOCK, BLOCK, FILTER_BUNDLES, BUNDLE_BREADTH)
    location_blended = jnp.einsum('gts,bsgd->btgd', masked, signal_blocks) + location_offsets.T[None, :, :, None]
    filtered_result = (conveyor_current * location_blended.reshape(WORD_TOTALITY, FILTER_BUNDLES * BUNDLE_BREADTH)).astype(jnp.bfloat16)
    middle = (sequence_entries.astype(jnp.float32) + split_sum(filtered_result, branch_emission_matrix, emission_rescalers, N_TP)).astype(jnp.bfloat16)
    ffn_in = normalize(middle, latter_norm_factor)
    hidden = (jax.nn.silu(rescaled_matmul(ffn_in, valve_matrix, valve_rescalers)) * rescaled_matmul(ffn_in, raising_matrix, raising_rescalers)).astype(jnp.bfloat16)
    return (middle.astype(jnp.float32) + split_sum(hidden, lowering_matrix, lowering_rescalers, N_TP)).astype(jnp.bfloat16)
```

```python
import functools

import jax
import jax.numpy as jnp
from jax import lax
from jax.experimental import pallas as pl
from jax.experimental.pallas import tpu as pltpu
from jax.sharding import PartitionSpec as P

EPS = 1e-06
MESH = pl.DeviceIdType.MESH
BF = jnp.bfloat16
F32 = jnp.float32


def layer_kernel(
    dims,
    x_in, g1, wc_in, wb_in, we_in, wv_in, wr_in, wl_in,
    sc, sb, gb, loc, offs, g2, sv, sr,
    out,
    wc, wb, we, wv, wr, wl,
    xa, xm, nrm, car, sgn, gat, hid, sq, part, half, rcore, rx, rz, dx_in, dz_in,
    p1s, p1r, p1l, p2s, p2r, ags, agr, sqs, sqr, rss, rsr,
):
    rows, width, chan, block_len, group_width, total_chan = dims
    fs = lax.axis_index("fs")
    c = lax.axis_index("tp")
    x = fs % 2
    y = (fs // 2) % 2
    zl = (fs // 4) % 2
    zh = fs // 8
    ai = x + 2 * zl

    def dev(dx=0, dy=0, dzl=0, dzh=0, dc=0):
        nx = 1 - x if dx else x
        ny = 1 - y if dy else y
        nzl = 1 - zl if dzl else zl
        nzh = 1 - zh if dzh else zh
        nc = 1 - c if dc else c
        return {"fs": nzh * 8 + nzl * 4 + ny * 2 + nx, "tp": nc}

    def blk(da):
        return (1 - x if da & 1 else x) + 2 * (1 - zl if da & 2 else zl)

    peers = [dev(dx=da & 1, dzl=da & 2, dc=dc) for da in range(4) for dc in range(2) if da or dc]
    peers += [dev(dy=1), dev(dzh=1)]
    barrier = pltpu.get_barrier_semaphore()
    for peer in peers:
        pl.semaphore_signal(barrier, inc=1, device_id=peer, device_id_type=MESH)
    pl.semaphore_wait(barrier, len(peers))

    def rcopy(src, dst, ss, rs, to):
        return pltpu.make_async_remote_copy(
            src_ref=src, dst_ref=dst, send_sem=ss, recv_sem=rs, device_id=to, device_id_type=MESH
        )

    pending = []

    def go(copy):
        copy.start()
        pending.append(copy)
        return copy

    ins = (wc_in, wb_in, we_in, wv_in, wr_in, wl_in)
    dst = (wc, wb, we, wv, wr, wl)
    rowwise = (False, False, True, False, False, True)

    def cell(m):
        if rowwise[m]:
            lanes = ins[m].shape[2]
            return dst[m].at[zh, zl, :, pl.ds(pl.multiple_of((y * 2 + x) * lanes, lanes), lanes)]
        return dst[m].at[zh, zl, y, x]

    def plane(m, a, b):
        if rowwise[m]:
            lanes = 2 * ins[m].shape[2]
            return dst[m].at[a, :, :, pl.ds(pl.multiple_of(b * lanes, lanes), lanes)]
        return dst[m].at[a, :, b]

    first = {}
    second = {}

    def phase1(m):
        local = pltpu.make_async_copy(ins[m].at[ai], cell(m), p1l.at[m])
        local.start()
        copies = [
            go(rcopy(ins[m].at[blk(da)], cell(m), p1s.at[m, da - 1], p1r.at[m, da - 1], dev(dx=da & 1, dzl=da & 2)))
            for da in (3, 1, 2)
        ]
        first[m] = (local, copies)

    def phase2(m):
        local, copies = first[m]
        local.wait()
        for copy in copies:
            copy.wait_recv()
        own = plane(m, zh, y)
        zcopy = go(rcopy(own, own, p2s.at[m, 0], p2r.at[m, 0], dev(dzh=1)))
        ycopy = go(rcopy(own, own, p2s.at[m, 1], p2r.at[m, 1], dev(dy=1)))
        second[m] = [zcopy, ycopy]

    def forward(m):
        second[m][0].wait_recv()
        far = plane(m, 1 - zh, y)
        second[m].append(go(rcopy(far, far, p2s.at[m, 2], p2r.at[m, 2], dev(dy=1))))

    def ready(m):
        second[m][1].wait_recv()
        second[m][2].wait_recv()

    hr = rows // 2
    top, bottom = pl.ds(0, hr), pl.ds(hr, hr)

    def gather_start(buf, k):
        own = buf.at[c, ai]
        z = go(rcopy(own, own, ags.at[k, 0], agr.at[k, 0], dev(dzl=1)))
        xx = go(rcopy(own, own, ags.at[k, 1], agr.at[k, 1], dev(dx=1)))
        core = go(rcopy(own, own, ags.at[k, 2], agr.at[k, 2], dev(dc=1)))
        return [z, xx, core]

    def gather_forward(buf, k, st):
        z, xx, core = st
        z.wait_recv()
        zb = buf.at[c, blk(2)]
        zbt = buf.at[c, blk(2), top]
        d1 = go(rcopy(zbt, zbt, ags.at[k, 3], agr.at[k, 3], dev(dx=1)))
        c1 = go(rcopy(zb, zb, ags.at[k, 4], agr.at[k, 4], dev(dc=1)))
        xx.wait_recv()
        xb = buf.at[c, blk(1)]
        xbb = buf.at[c, blk(1), bottom]
        d2 = go(rcopy(xbb, xbb, ags.at[k, 5], agr.at[k, 5], dev(dzl=1)))
        c2 = go(rcopy(xb, xb, ags.at[k, 6], agr.at[k, 6], dev(dc=1)))
        st += [d1, c1, d2, c2]

    def gather_last(buf, k, st):
        d1, c1, d2, c2 = st[3:]
        d1.wait_recv()
        d2.wait_recv()
        db = buf.at[c, blk(3)]
        st.append(go(rcopy(db, db, ags.at[k, 7], agr.at[k, 7], dev(dc=1))))

    def norm_block(buf, gain, b):
        total = jnp.zeros((rows, 1), F32)
        for h in range(2):
            v = buf[h, b].astype(F32)
            total = total + jnp.sum(v * v, axis=-1, keepdims=True)
        factor = lax.rsqrt(total / (2 * width) + EPS)
        for h in range(2):
            nrm[h] = (buf[h, b].astype(F32) * factor * gain[h]).astype(BF)

    def project(w):
        n = w.shape[-1]
        return jnp.dot(nrm[0], w[0].reshape(width, n), preferred_element_type=F32) + jnp.dot(
            nrm[1], w[1].reshape(width, n), preferred_element_type=F32
        )

    def emit(src, w, b):
        v = src[b]
        for h in range(2):
            for q in range(2):
                n = w.shape[-1]
                part[h, b, :, q * n:(q + 1) * n] = jnp.dot(
                    v, w[h, q], preferred_element_type=F32
                ).astype(BF)

    def scatter(k, src, w):
        cores = {}
        order = (3, 2, 1, 0)
        for i, da in enumerate(order):
            b = blk(da)
            emit(src, w, b)
            cores[da] = rcopy(part.at[1 - c, b], rcore.at[k, b], rss.at[k, i], rsr.at[k, i], dev(dc=1))
            cores[da].start()

        def combine(da):
            b = blk(da)
            cores[da].wait_recv()
            half[k, b] = (part[c, b].astype(F32) + rcore[k, b].astype(F32)).astype(BF)

        combine(3)
        dxc = go(rcopy(half.at[k, blk(3), top], dx_in.at[k], rss.at[k, 4], rsr.at[k, 4], dev(dx=1)))
        dzc = go(rcopy(half.at[k, blk(3), bottom], dz_in.at[k], rss.at[k, 5], rsr.at[k, 5], dev(dzl=1)))
        combine(2)
        zb = blk(2)
        z1 = go(rcopy(half.at[k, zb, bottom], rz.at[k, bottom], rss.at[k, 6], rsr.at[k, 6], dev(dzl=1)))
        combine(1)
        xb = blk(1)
        x1 = go(rcopy(half.at[k, xb, top], rx.at[k, top], rss.at[k, 7], rsr.at[k, 7], dev(dx=1)))
        dxc.wait_recv()
        half[k, zb, :hr] = (half[k, zb, :hr].astype(F32) + dx_in[k].astype(F32)).astype(BF)
        z2 = go(rcopy(half.at[k, zb, top], rz.at[k, top], rss.at[k, 8], rsr.at[k, 8], dev(dzl=1)))
        dzc.wait_recv()
        half[k, xb, hr:] = (half[k, xb, hr:].astype(F32) + dz_in[k].astype(F32)).astype(BF)
        x2 = go(rcopy(half.at[k, xb, bottom], rx.at[k, bottom], rss.at[k, 9], rsr.at[k, 9], dev(dx=1)))
        cores[0].wait_recv()
        for da in order:
            cores[da].wait_send()
        own = part[c, ai].astype(F32) + rcore[k, ai].astype(F32)
        for copy in (z1, x1, z2, x2):
            copy.wait_recv()
        return own + rz[k].astype(F32) + rx[k].astype(F32)

    mine = pltpu.make_async_copy(x_in, xa.at[c, ai], p1l.at[6])
    mine.start()
    phase1(0)
    phase1(1)
    mine.wait()
    st1 = gather_start(xa, 0)
    phase2(0)
    phase2(1)
    gather_forward(xa, 0, st1)
    for m in (2, 3, 4, 5):
        phase1(m)
    gather_last(xa, 0, st1)
    forward(0)
    forward(1)
    for m in (2, 3, 4, 5):
        phase2(m)
    ready(0)
    ready(1)
    core_of = {0: 2, 2: 4, 1: 6, 3: 7}
    slot = ai * 2 + c
    for da in (0, 2, 1, 3):
        b = blk(da)
        st1[core_of[da]].wait_recv()
        norm_block(xa, g1, b)
        car[b] = jax.nn.gelu(project(wc) * sc[...])
        signal = jax.nn.gelu(project(wb) * sb[...])
        sgn[b] = (signal * gb[...]).astype(BF)
        sq[slot, b] = lax.dot_general(
            jnp.ones((8, chan), F32), signal * signal, (((1,), (1,)), ((), ())),
            precision=lax.Precision.HIGHEST, preferred_element_type=F32,
        )
    squares = []
    for da in range(4):
        for dc in range(2):
            if da or dc:
                i = da * 2 + dc - 1
                squares.append(
                    go(rcopy(sq.at[slot], sq.at[slot], sqs.at[i], sqr.at[i], dev(dx=da & 1, dzl=da & 2, dc=dc)))
                )
    forward(2)
    ready(2)
    for copy in squares:
        copy.wait_recv()
    groups = chan // group_width
    lower = lax.broadcasted_iota(jnp.int32, (block_len, block_len), 0) >= lax.broadcasted_iota(
        jnp.int32, (block_len, block_len), 1
    )
    lane = lax.broadcasted_iota(jnp.int32, (block_len, chan), 1)
    for da in range(4):
        b = blk(da)
        total = sq[0, b]
        for i in range(1, 8):
            total = total + sq[i, b]
        factor = lax.rsqrt(total / total_chan + EPS)
        for s in range(rows // block_len):
            span = slice(s * block_len, (s + 1) * block_len)
            values = sgn[b, span]
            mixed = jnp.zeros((block_len, chan), F32)
            for g in range(groups):
                mat = jnp.where(lower, loc[g].astype(F32), 0.0) * factor[0:1, span]
                one = jnp.dot(mat.astype(BF), values, preferred_element_type=F32)
                inside = (lane >= g * group_width) & (lane < (g + 1) * group_width)
                mixed = jnp.where(inside, one, mixed)
            gat[b, span] = (car[b, span] * (mixed + offs[...])).astype(BF)
    summed = scatter(0, gat, we)
    xm[c, ai] = (xa[c, ai].astype(F32) + summed).astype(BF)
    st2 = gather_start(xm, 1)
    forward(3)
    forward(4)
    gather_forward(xm, 1, st2)
    gather_last(xm, 1, st2)
    ready(3)
    ready(4)
    for da in (0, 2, 1, 3):
        b = blk(da)
        st2[core_of[da]].wait_recv()
        norm_block(xm, g2, b)
        gate = project(wv) * sv[...]
        up = project(wr) * sr[...]
        hid[b] = (jax.nn.silu(gate) * up).astype(BF)
    forward(5)
    ready(5)
    summed = scatter(1, hid, wl)
    out[...] = (xm[c, ai].astype(F32) + summed).astype(BF)
    for copy in pending:
        copy.wait_send()


def on_device_fused(
    sequence_entries, former_norm_factor, conveyor_matrix, conveyor_rescalers,
    blend_value_matrix, blend_rescalers, blend_norm_factor, location_matrices,
    location_offsets, branch_emission_matrix, emission_rescalers, latter_norm_factor,
    valve_matrix, valve_rescalers, raising_matrix, raising_rescalers,
    lowering_matrix, lowering_rescalers,
):
    parts = 4
    fs = lax.axis_index("fs")
    ai = fs % 2 + 2 * ((fs // 4) % 2)
    rows, width = sequence_entries.shape
    depth = conveyor_matrix.shape[0]
    chan = conveyor_matrix.shape[1] // parts
    ff = valve_matrix.shape[1] // parts
    groups = location_matrices.shape[0] // parts
    block_len = location_matrices.shape[1]
    group_width = chan // groups
    total_chan = conveyor_matrix.shape[1] * lax.axis_size("tp")
    cols = branch_emission_matrix.shape[1]

    def by_columns(w):
        return w.astype(BF).reshape(depth, parts, -1).transpose(1, 0, 2)

    def by_rows(w, scale):
        return (w * scale[None, :]).astype(BF).reshape(parts, -1, cols)

    def own(v):
        n = v.shape[0] // parts
        return lax.dynamic_slice_in_dim(v, ai * n, n, 0)

    offs = jnp.repeat(own(location_offsets), group_width, axis=0).T
    args = (
        sequence_entries,
        former_norm_factor.reshape(2, 1, width),
        by_columns(conveyor_matrix),
        by_columns(blend_value_matrix),
        by_rows(branch_emission_matrix, emission_rescalers),
        by_columns(valve_matrix),
        by_columns(raising_matrix),
        by_rows(lowering_matrix, lowering_rescalers),
        own(conveyor_rescalers)[None],
        own(blend_rescalers)[None],
        own(blend_norm_factor)[None],
        own(location_matrices),
        offs,
        latter_norm_factor.reshape(2, 1, width),
        own(valve_rescalers)[None],
        own(raising_rescalers)[None],
    )
    vm = pltpu.VMEM
    dma = pltpu.SemaphoreType.DMA
    cube = (2, 2, 2, 2, depth)
    scratch = [
        vm(cube + (chan,), BF), vm(cube + (chan,), BF), vm((2, 2, chan, 4 * cols), BF),
        vm(cube + (ff,), BF), vm(cube + (ff,), BF), vm((2, 2, ff, 4 * cols), BF),
        vm((2, 4, rows, width), BF), vm((2, 4, rows, width), BF), vm((2, rows, width), BF),
        vm((4, rows, chan), F32), vm((4, rows, chan), BF), vm((4, rows, chan), BF),
        vm((4, rows, ff), BF), vm((8, 4, 8, rows), F32),
        vm((2, 4, rows, width), BF), vm((2, 4, rows, width), BF), vm((2, 4, rows, width), BF),
        vm((2, rows, width), BF), vm((2, rows, width), BF),
        vm((2, rows // 2, width), BF), vm((2, rows // 2, width), BF),
        dma((6, 3)), dma((6, 3)), dma((7,)), dma((6, 3)), dma((6, 3)),
        dma((2, 8)), dma((2, 8)), dma((7,)), dma((7,)), dma((2, 10)), dma((2, 10)),
    ]
    dims = (rows, width, chan, block_len, group_width, total_chan)
    return pl.pallas_call(
        functools.partial(layer_kernel, dims),
        out_shape=jax.ShapeDtypeStruct((rows, width), BF),
        in_specs=[pl.BlockSpec(memory_space=pltpu.VMEM)] * len(args),
        out_specs=pl.BlockSpec(memory_space=pltpu.VMEM),
        scratch_shapes=scratch,
        compiler_params=pltpu.CompilerParams(
            collective_id=0, has_side_effects=True, vmem_limit_bytes=63000000
        ),
    )(*args)


def normalize(rows, gain):
    values = rows.astype(jnp.float32)
    factor = lax.rsqrt(jnp.mean(values * values, axis=-1, keepdims=True) + EPS)
    return (values * factor * gain).astype(jnp.bfloat16)


def elementwise_plus(left_rows, pieces):
    return (
        jnp.dot(left_rows, pieces[0], preferred_element_type=jnp.float32),
        jnp.dot(left_rows, pieces[1], preferred_element_type=jnp.float32),
    )


def project_cols(left_rows, scales, piece):
    return jnp.dot(left_rows, piece, preferred_element_type=jnp.float32) * scales


def on_device(
    sequence_entries,
    former_norm_factor,
    conveyor_matrix,
    conveyor_rescalers,
    blend_value_matrix,
    blend_rescalers,
    blend_norm_factor,
    location_matrices,
    location_offsets,
    branch_emission_matrix,
    emission_rescalers,
    latter_norm_factor,
    valve_matrix,
    valve_rescalers,
    raising_matrix,
    raising_rescalers,
    lowering_matrix,
    lowering_rescalers,
):
    out_scales, down_scales = (
        lax.all_gather(emission_rescalers, "fs", axis=0, tiled=True),
        lax.all_gather(lowering_rescalers, "fs", axis=0, tiled=True),
    )
    full_rows = lax.all_gather(sequence_entries, "tp", axis=1, tiled=True)
    own_width = sequence_entries.shape[1]
    own_start = lax.axis_index("tp") * own_width
    standardized_source = normalize(full_rows, former_norm_factor)
    conveyor_prior, stream_prior = elementwise_plus(
        standardized_source,
        (
            lax.all_gather(conveyor_matrix.astype(jnp.bfloat16), "fs", axis=0, tiled=True),
            lax.all_gather(blend_value_matrix.astype(jnp.bfloat16), "fs", axis=0, tiled=True),
        ),
    )
    conveyor_current = jax.nn.gelu(conveyor_prior * conveyor_rescalers)
    signal = jax.nn.gelu(stream_prior * blend_rescalers)
    total_sq = lax.psum(jnp.sum(signal * signal, axis=1), "tp")
    channels = signal.shape[1] * lax.axis_size("tp")
    signal_norm = (
        signal * lax.rsqrt(total_sq / channels + EPS)[:, None] * blend_norm_factor
    ).astype(jnp.bfloat16)
    local_groups = location_matrices.shape[0]
    block_len = location_matrices.shape[1]
    group_width = signal.shape[1] // local_groups
    lower_mask = jnp.tril(jnp.ones((block_len, block_len), bool))
    masked = jnp.where(lower_mask[None], location_matrices, jnp.zeros((), jnp.bfloat16))
    signal_blocks = signal_norm.reshape(-1, block_len, local_groups, group_width)
    location_blended = jnp.einsum(
        "gts,bsgd->btgd", masked, signal_blocks, preferred_element_type=jnp.float32
    )
    location_blended = location_blended + location_offsets.T[None, :, :, None]
    filtered_result = (conveyor_current * location_blended.reshape(conveyor_current.shape)).astype(
        jnp.bfloat16
    )
    mixer_terms = project_cols(
        filtered_result,
        out_scales,
        lax.all_gather(branch_emission_matrix.astype(jnp.bfloat16), "fs", axis=1, tiled=True),
    )
    summed = lax.psum(mixer_terms.astype(jnp.bfloat16), "tp").astype(jnp.float32)
    mid_rows = (full_rows.astype(jnp.float32) + summed).astype(jnp.bfloat16)
    mid_own = lax.dynamic_slice_in_dim(mid_rows, own_start, own_width, 1)
    ffn_in = normalize(mid_rows, latter_norm_factor)
    gate_half = valve_matrix.astype(jnp.bfloat16)
    up_half = raising_matrix.astype(jnp.bfloat16)
    whole_gate, whole_up = (
        lax.all_gather(gate_half, "fs", axis=0, tiled=True),
        lax.all_gather(up_half, "fs", axis=0, tiled=True),
    )
    pre_gate = jnp.dot(ffn_in, whole_gate, preferred_element_type=jnp.float32)
    pre_up = jnp.dot(ffn_in, whole_up, preferred_element_type=jnp.float32)
    hidden = (jax.nn.silu(pre_gate * valve_rescalers) * (pre_up * raising_rescalers)).astype(
        jnp.bfloat16
    )
    ffn_terms = project_cols(
        hidden,
        down_scales,
        lax.all_gather(lowering_matrix.astype(jnp.bfloat16), "fs", axis=1, tiled=True),
    )
    ffn_share = lax.psum_scatter(
        ffn_terms.astype(jnp.bfloat16), "tp", scatter_dimension=1, tiled=True
    ).astype(jnp.float32)
    return (mid_own.astype(jnp.float32) + ffn_share).astype(jnp.bfloat16)


def solution(mesh):
    sizes = dict(mesh.shape)
    fused = sizes["tp"] == 2 and sizes["fs"] == 16
    return jax.shard_map(
        on_device_fused if fused else on_device,
        mesh=mesh,
        in_specs=(
            P("fs", "tp"),
            P(),
            P("fs", "tp"),
            P("tp"),
            P("fs", "tp"),
            P("tp"),
            P("tp"),
            P("tp", None, None),
            P("tp", None),
            P("tp", "fs"),
            P("fs"),
            P(),
            P("fs", "tp"),
            P("tp"),
            P("fs", "tp"),
            P("tp"),
            P("tp", "fs"),
            P("fs"),
        ),
        out_specs=P("fs", "tp"),
        check_vma=False,
    )
```
